32 devices in a mesh: sp: 16 (over z, y, core), dp: 2 (over x).
Axes of the slice: x: 2, y: 2, z: 4, core: 2. Of those that a mesh axis runs over, the one named last changes fastest.
Arguments:
- tokens: bfloat16 [2, 2048, 1024], P('dp', 'sp'), may hold values from -6 to 6
- proj_gate: bfloat16 [1024, 1024], P(('sp', 'dp')), may hold values from -0.1875 to 0.1875
- proj_value: bfloat16 [1024, 1024], P(('sp', 'dp')), may hold values from -0.1875 to 0.1875
- norm_gain: float32 [1024], replicated, may hold values from 0.1 to 1.9
- mix_weight: bfloat16 [4, 1024, 1024], P(None, 'dp'), may hold values from -0.1875 to 0.1875
- mix_bias: float32 [4, 1024], replicated, may hold values from 0.1 to 1.9
- proj_out: bfloat16 [1024, 1024], P(('sp', 'dp')), may hold values from -0.1875 to 0.1875
Outputs:
- mixed: bfloat16 [2, 2048, 1024], P('dp', 'sp')
The draws below stay inside these ranges and needn't reach their ends.
All inputs are finite; a program needn't handle non-finite values.
Results may differ from the reference program's by a relative error of at most 0.015.
Values may be sent and summed in bfloat16 or wider, within the bound.
A program may use at most 64 MiB of HBM per device.

```python
import jax
import jax.numpy as jnp
from jax import lax

D = 1024
WIDTH = 1024
HEAD_DIM = 256
BLOCK = 1024
SPAN = 64
HEADS = 4
TOKENS = 2048
SEQS = 2


def steps_of(key, dims, split, least, largest):
    level, own = 1.0, jax.random.fold_in(key, 6)
    for dim, blocks in split:
        heights = jnp.exp(jax.random.uniform(jax.random.fold_in(own, dim), (blocks,), jnp.float32, least / len(split), largest / len(split)))
        level = level * jnp.repeat(heights, dims[dim] // blocks).reshape([-1 if axis == dim else 1 for axis in range(len(dims))])
    return level


def bell_draw(rng, shape, deviation, reach, shards=(), kind=jnp.bfloat16):
    level = steps_of(rng, shape, shards, -0.22, 0.18) if shards else 1.0
    drawn = jax.random.normal(rng, shape, jnp.float32) * deviation * level
    return jnp.minimum(jnp.maximum(drawn, -reach), reach).astype(kind)


def setup_inputs(seed: int = 0) -> dict:
    splits = jax.random.split(jax.random.key(seed), 8)
    tokens = bell_draw(splits[0], (SEQS, TOKENS, D), 1.0, 6.0, ((0, 2), (1, 16)))
    proj_gate = bell_draw(splits[1], (D, WIDTH), D ** -0.5, 0.1875, ((0, 32),))
    proj_value = bell_draw(splits[2], (D, WIDTH), D ** -0.5, 0.1875, ((0, 32),))
    norm_gain = jnp.clip(1.0 + 0.18 * jax.random.normal(splits[3], (WIDTH,), jnp.float32), 0.1, 1.9)
    mix_weight = bell_draw(splits[4], (HEADS, BLOCK, BLOCK), BLOCK ** -0.5, 0.1875, ((1, 2),))
    mix_bias = jnp.clip(1.0 + 0.18 * jax.random.normal(splits[5], (HEADS, BLOCK), jnp.float32), 0.1, 1.9)
    proj_out = bell_draw(splits[6], (WIDTH, D), WIDTH ** -0.5, 0.1875, ((0, 32),))
    return {"tokens": tokens, "proj_gate": proj_gate, "proj_value": proj_value, "norm_gain": norm_gain, "mix_weight": mix_weight, "mix_bias": mix_bias, "proj_out": proj_out}


def reference(tokens, proj_gate, proj_value, norm_gain, mix_weight, mix_bias, proj_out):
    flat = tokens.reshape(-1, D)
    u_part = jnp.dot(flat, proj_gate, preferred_element_type=jnp.float32).astype(jnp.bfloat16)
    v_part = jnp.dot(flat, proj_value, preferred_element_type=jnp.float32).astype(jnp.bfloat16)
    v_float = v_part.astype(jnp.float32)
    centre = lax.optimization_barrier(jnp.mean(v_float, axis=-1, keepdims=True))
    spread = lax.optimization_barrier(jnp.mean(jnp.square(v_float - centre), axis=-1, keepdims=True))
    normed = ((v_float - centre) * lax.rsqrt(spread + 1e-05) * norm_gain).astype(jnp.bfloat16)
    blocks = normed.reshape(SEQS, TOKENS // BLOCK, BLOCK, HEADS, HEAD_DIM).astype(jnp.float32)
    index = jnp.arange(BLOCK, dtype=jnp.int32)
    allowed = index[None, :] // SPAN <= index[:, None] // SPAN
    masked = jnp.where(allowed[None], mix_weight.astype(jnp.float32), 0.0)
    spatial = jnp.einsum('hij,snjhc->snihc', masked, blocks, precision=lax.Precision.HIGHEST)
    spatial = spatial + jnp.transpose(mix_bias)[None, None, :, :, None]
    spatial = spatial.astype(jnp.bfloat16).reshape(-1, WIDTH)
    gated = (u_part.astype(jnp.float32) * spatial.astype(jnp.float32)).astype(jnp.bfloat16)
    result = jnp.dot(gated, proj_out, preferred_element_type=jnp.float32).astype(jnp.bfloat16)
    return result.reshape(SEQS, TOKENS, D)
```

```python
import functools

import jax
import jax.numpy as jnp
from jax import lax
from jax.experimental import pallas as pl
from jax.experimental.pallas import tpu as pltpu
from jax.sharding import PartitionSpec as P

HEAD_DIM = 256
SPAN = 64
EPS = 1e-05
NT = (((1,), (1,)), ((), ()))


def dot_nt(left, right):
    return lax.dot_general(left, right, NT, preferred_element_type=jnp.float32)


def kernel(n_sp, n_dp, tok, wg, wv, gain, mix, bias, wo, out,
           toks, wbuf, mbuf, stats, gat, ubuf, vbuf, osend,
           tok_s, tok_r, w_s, w_r, m_l, m_s, m_r, st_s, st_r, g_s, g_r, o_s, o_r):
    rows, model = tok.shape
    width = gain.shape[1]
    block = mix.shape[2]
    n = block // rows
    chips = n // 2
    cols = width // n
    depth = wg.shape[0]
    mrows = mix.shape[1]
    mhalf = mrows // 2
    total = n_sp * n_dp
    sp, dp = lax.axis_index("sp"), lax.axis_index("dp")
    p = lax.rem(sp, n)
    base = sp - p
    chip, core = lax.div(p, 2), lax.rem(p, 2)
    partner = {"sp": base + chip * 2 + 1 - core, "dp": dp}
    me = sp * n_dp + dp
    head = lax.div(p * cols, HEAD_DIM)

    def copy(src, dst, ssem, rsem, device):
        return pltpu.make_async_remote_copy(
            src_ref=src, dst_ref=dst, send_sem=ssem, recv_sem=rsem,
            device_id=device, device_id_type=pl.DeviceIdType.MESH)

    def device(line):
        return {"sp": lax.div(line, n_dp), "dp": lax.rem(line, n_dp)}

    barrier = pltpu.get_barrier_semaphore()

    @pl.loop(1, total)
    def _(off):
        pl.semaphore_signal(barrier, inc=1, device_id=device(lax.rem(me + off, total)),
                            device_id_type=pl.DeviceIdType.MESH)

    pl.semaphore_wait(barrier, total - 1)

    def slot_of(k, side):
        return lax.rem(chip + chips - k, chips) * 2 + side

    def spread(src, buf, ssem, rsem):
        started = []
        for k in range(1, chips):
            peer = base + lax.rem(chip + k, chips) * 2 + core
            started.append(copy(src, buf.at[p], ssem.at[k], rsem.at[p], {"sp": peer, "dp": dp}))
        started.append(copy(src, buf.at[p], ssem.at[0], rsem.at[p], partner))
        for one in started:
            one.start()
        return started

    def relay(k, buf, ssem, rsem):
        slot = slot_of(k, core)
        one = copy(buf.at[slot], buf.at[slot], ssem.at[chips - 1 + k], rsem.at[slot], partner)
        one.wait_recv()
        one.start()
        return one

    def arrive(k, buf, ssem, rsem):
        slot = slot_of(k, 1 - core)
        copy(buf.at[slot], buf.at[slot], ssem.at[0], rsem.at[slot], partner).wait_recv()

    sent = spread(tok, toks, tok_s, tok_r)

    def weight_sends(i, w):
        @pl.loop(1, total)
        def _(off):
            to = device(lax.rem(me + off, total))
            start = pl.multiple_of(lax.rem(to["sp"], n) * cols, cols)
            copy(w.at[:, pl.ds(start, cols)], wbuf.at[i, me], w_s.at[i], w_r.at[i], to).start()

    weight_sends(1, wv)
    weight_sends(0, wg)
    mine = pltpu.make_async_copy(
        mix.at[head], mbuf.at[pl.ds(pl.multiple_of(dp * mrows, mrows), mrows)], m_l)
    mine.start()
    for k in range(1, n_dp):
        to = lax.rem(dp + k, n_dp)
        span = pl.ds(pl.multiple_of(dp * mrows + core * mhalf, mhalf), mhalf)
        one = copy(mix.at[head, pl.ds(pl.multiple_of(core * mhalf, mhalf), mhalf)], mbuf.at[span],
                   m_s.at[k], m_r.at[dp * 2 + core], {"sp": sp, "dp": to})
        one.start()
        sent.append(one)
    weight_sends(2, wo)

    own = pl.ds(pl.multiple_of(p * cols, cols), cols)
    toks[p] = tok[...]
    for i, w in enumerate((wg, wv, wo)):
        wbuf[i, me] = w[:, own]

    for k in range(1, chips):
        sent.append(relay(k, toks, tok_s, tok_r))

    def weight_wait(sem, i):
        part = wbuf.at[i, pl.ds(0, total - 1)]
        pltpu.make_async_copy(part, part, sem.at[i]).wait()

    def columns_t(i):
        flat = wbuf[i].astype(jnp.float32).reshape(total * depth, cols)
        return jnp.transpose(flat).astype(jnp.bfloat16)

    weight_wait(w_r, 1)
    weight_wait(w_r, 0)
    both = jnp.concatenate([columns_t(0), columns_t(1)], axis=0)
    pair = 2 * rows
    for k in range(chips):
        arrive(k, toks, tok_s, tok_r)
        at = lax.rem(chip + chips - k, chips)
        part = toks[pl.ds(at * 2, 2)].reshape(pair, model)
        result = dot_nt(both, part)
        lanes = pl.ds(pl.multiple_of(at * pair, pair), pair)
        ubuf[:, lanes] = result[:cols].astype(jnp.bfloat16)
        v = result[cols:].astype(jnp.bfloat16).astype(jnp.float32)
        vbuf[:, lanes] = v
        total_v = jnp.sum(v, axis=0, keepdims=True)
        away = v - total_v * (1.0 / cols)
        stats[p, 0:1, lanes] = total_v
        stats[p, 1:2, lanes] = jnp.sum(away * away, axis=0, keepdims=True)

    for k in range(1, n):
        peer = base + lax.rem(p + k, n)
        one = copy(stats.at[p], stats.at[p], st_s.at[k], st_r.at[p], {"sp": peer, "dp": dp})
        one.start()
        sent.append(one)

    mine.wait()
    for k in range(1, n_dp):
        of = lax.rem(dp + n_dp - k, n_dp)
        span = pl.ds(pl.multiple_of(of * mrows + core * mhalf, mhalf), mhalf)
        one = copy(mbuf.at[span], mbuf.at[span], m_s.at[n_dp - 1 + k], m_r.at[of * 2 + core], partner)
        one.wait_recv()
        one.start()
        sent.append(one)
    for k in range(1, n_dp):
        of = lax.rem(dp + n_dp - k, n_dp)
        span = pl.ds(pl.multiple_of(of * mrows + (1 - core) * mhalf, mhalf), mhalf)
        copy(mbuf.at[span], mbuf.at[span], m_s.at[0], m_r.at[of * 2 + 1 - core], partner).wait_recv()

    gain_t = jnp.transpose(jnp.broadcast_to(gain[:, own], (cols, cols)))[:, 0:1]
    for k in range(1, n):
        slot = lax.rem(p + n - k, n)
        copy(stats.at[slot], stats.at[slot], st_s.at[0], st_r.at[slot], partner).wait_recv()
    sums = [stats[q, 0:1, :] for q in range(n)]
    mean = functools.reduce(jnp.add, sums) * (1.0 / width)
    square = jnp.zeros_like(mean)
    for q in range(n):
        gap = sums[q] * (1.0 / cols) - mean
        square = square + stats[q, 1:2, :] + cols * (gap * gap)
    scale = lax.rsqrt(square * (1.0 / width) + EPS)
    normed = ((vbuf[...] - mean) * scale * gain_t).astype(jnp.bfloat16)

    tile = pair
    row = lax.broadcasted_iota(jnp.int32, (tile, tile), 0) // SPAN
    col = lax.broadcasted_iota(jnp.int32, (tile, tile), 1) // SPAN
    bias_row = bias[pl.ds(head, 1), :]
    for t in range(block // tile):
        lo, hi = t * tile, (t + 1) * tile
        diag = mbuf[lo:hi, lo:hi]
        diag = jnp.where(col <= row, diag.astype(jnp.float32), 0.0).astype(jnp.bfloat16)
        mixed = dot_nt(normed[:, lo:hi], diag)
        if t:
            mixed = mixed + dot_nt(normed[:, :lo], mbuf[lo:hi, :lo])
        mixed = (mixed + bias_row[:, lo:hi]).astype(jnp.bfloat16).astype(jnp.float32)
        gat[p, :, lo:hi] = (ubuf[:, lo:hi].astype(jnp.float32) * mixed).astype(jnp.bfloat16)

    sent += spread(gat.at[p], gat, g_s, g_r)
    weight_wait(w_r, 2)
    wo_t = columns_t(2)
    for k in range(1, chips):
        sent.append(relay(k, gat, g_s, g_r))
    for k in range(chips):
        arrive(k, gat, g_s, g_r)

    for k in range(chips):
        at = lax.rem(chip + 1 + k, chips)
        lanes = pl.ds(pl.multiple_of(at * pair, pair), pair)
        right = gat[:, :, lanes].reshape(width, pair)
        result = jnp.dot(wo_t, right, preferred_element_type=jnp.float32)
        turned = jnp.transpose(result).astype(jnp.bfloat16)
        osend[pl.ds(at * 2, 2)] = turned.reshape(2, rows, cols)
        if k < chips - 1:
            for side in range(2):
                one = copy(osend.at[at * 2 + side], out.at[:, own], o_s.at[2 * k + side], o_r.at[p],
                           {"sp": base + at * 2 + side, "dp": dp})
                one.start()
                sent.append(one)
    one = copy(osend.at[chip * 2 + 1 - core], out.at[:, own], o_s.at[n - 1], o_r.at[p], partner)
    one.start()
    sent.append(one)
    out[:, own] = osend[p]
    for k in range(1, n):
        slot = lax.rem(p + n - k, n)
        there = out.at[:, pl.ds(pl.multiple_of(slot * cols, cols), cols)]
        copy(osend.at[0], there, o_s.at[0], o_r.at[slot], partner).wait_recv()
    for one in sent:
        one.wait_send()
    for i in range(3):
        weight_wait(w_s, i)


def body(n_sp, n_dp, tokens, proj_gate, proj_value, norm_gain, mix_weight, mix_bias, proj_out):
    rows, model = tokens.shape[1:]
    width = norm_gain.shape[0]
    block = mix_weight.shape[2]
    n = block // rows
    cols = width // n
    depth = proj_gate.shape[0]
    total = n_sp * n_dp
    vmem = pl.BlockSpec(memory_space=pltpu.VMEM)
    dma = pltpu.SemaphoreType.DMA
    result = pl.pallas_call(
        functools.partial(kernel, n_sp, n_dp),
        out_shape=jax.ShapeDtypeStruct((rows, model), jnp.bfloat16),
        in_specs=[vmem, vmem, vmem, vmem, pl.BlockSpec(memory_space=pl.ANY), vmem, vmem],
        out_specs=vmem,
        scratch_shapes=[
            pltpu.VMEM((n, rows, model), jnp.bfloat16),
            pltpu.VMEM((3, total, depth, cols), jnp.bfloat16),
            pltpu.VMEM((block, block), jnp.bfloat16),
            pltpu.VMEM((n, 2, block), jnp.float32),
            pltpu.VMEM((n, cols, block), jnp.bfloat16),
            pltpu.VMEM((cols, block), jnp.bfloat16),
            pltpu.VMEM((cols, block), jnp.float32),
            pltpu.VMEM((n, rows, cols), jnp.bfloat16),
            dma((n,)), dma((n,)), dma((3,)), dma((3,)),
            dma, dma((2 * n_dp,)), dma((2 * n_dp,)),
            dma((n,)), dma((n,)), dma((n,)), dma((n,)), dma((n,)), dma((n,)),
        ],
        compiler_params=pltpu.CompilerParams(
            collective_id=0, has_side_effects=True, vmem_limit_bytes=32 * 1024 * 1024),
    )(tokens.reshape(rows, model), proj_gate, proj_value, norm_gain.reshape(1, width),
      mix_weight, mix_bias, proj_out)
    return result.reshape(1, rows, model)


def solution(mesh):
    return jax.shard_map(
        functools.partial(body, mesh.shape["sp"], mesh.shape["dp"]),
        mesh=mesh,
        in_specs=(
            P("dp", "sp", None),
            P(("sp", "dp"), None),
            P(("sp", "dp"), None),
            P(),
            P(None, "dp", None),
            P(),
            P(("sp", "dp"), None),
        ),
        out_specs=P("dp", "sp", None),
        check_vma=False,
    )
```

```python
import functools

import jax
import jax.numpy as jnp
from jax import lax
from jax.experimental import pallas as pl
from jax.experimental.pallas import tpu as pltpu
from jax.sharding import PartitionSpec as P

HEAD_DIM = 256
SPAN = 64
EPS = 1e-05
NT = (((1,), (1,)), ((), ()))


def dot_nt(left, right):
    return lax.dot_general(left, right, NT, preferred_element_type=jnp.float32)


def kernel(n_sp, n_dp, tok, wg, wv, gain_in, mix, bias_in, wo, out,
           toks, wloc, wbuf, mbuf, dbuf, gain, bias, stats, gat, ubuf, vbuf, osend,
           l_s, tok_s, tok_r, w_s, w_r, x_s, x_r, m_s, m_r, st_s, st_r, g_s, g_r, o_s, o_r):
    rows, model = tok.shape
    width = gain.shape[1]
    block = mix.shape[2]
    n = block // rows
    chips = n // 2
    cols = width // n
    depth = wg.shape[0]
    mrows = mix.shape[1]
    mhalf = mrows // 2
    pair = 2 * rows
    sp, dp = lax.axis_index("sp"), lax.axis_index("dp")
    p = lax.rem(sp, n)
    base = sp - p
    chip, core = lax.div(p, 2), lax.rem(p, 2)
    partner = {"sp": base + chip * 2 + 1 - core, "dp": dp}
    head = lax.div(p * cols, HEAD_DIM)
    own = pl.ds(pl.multiple_of(p * cols, cols), cols)
    mine = pl.ds(pl.multiple_of(dp * mrows, mrows), mrows)

    def copy(src, dst, ssem, rsem, device):
        return pltpu.make_async_remote_copy(
            src_ref=src, dst_ref=dst, send_sem=ssem, recv_sem=rsem,
            device_id=device, device_id_type=pl.DeviceIdType.MESH)

    def at_sp(index):
        return {"sp": index, "dp": dp}

    loads = [(wg, wloc.at[0]), (wv, wloc.at[1]), (wo, wloc.at[2]), (tok, toks.at[p]),
             (gain_in, gain), (bias_in, bias), (mix.at[head], mbuf.at[mine])]
    loads += [(w.at[:, own], wbuf.at[i, sp, dp]) for i, w in enumerate((wg, wv, wo))]
    loads = [pltpu.make_async_copy(src, dst, l_s.at[i]) for i, (src, dst) in enumerate(loads)]
    for one in loads:
        one.start()

    barrier = pltpu.get_barrier_semaphore()

    @pl.loop(1, n_sp)
    def _(off):
        pl.semaphore_signal(barrier, inc=1, device_id=at_sp(lax.rem(sp + off, n_sp)),
                            device_id_type=pl.DeviceIdType.MESH)

    for k in range(1, n_dp):
        pl.semaphore_signal(barrier, inc=1, device_id={"sp": sp, "dp": lax.rem(dp + k, n_dp)},
                            device_id_type=pl.DeviceIdType.MESH)
    pl.semaphore_wait(barrier, n_sp + n_dp - 2)
    for one in loads:
        one.wait()
    sent = []

    def start(one):
        one.start()
        sent.append(one)

    def slot_of(k, side):
        return lax.rem(chip + chips - k, chips) * 2 + side

    def spread(view, ssem, rsem):
        for k in range(1, chips):
            peer = base + lax.rem(chip + k, chips) * 2 + core
            start(copy(view(p), view(p), ssem(k), rsem(p), at_sp(peer)))
        start(copy(view(p), view(p), ssem(0), rsem(p), partner))

    def relay(k, view, ssem, rsem):
        slot = slot_of(k, core)
        one = copy(view(slot), view(slot), ssem(chips - 1 + k), rsem(slot), partner)
        one.wait_recv()
        start(one)

    def arrive(k, view, ssem, rsem):
        slot = slot_of(k, 1 - core)
        copy(view(slot), view(slot), ssem(0), rsem(slot), partner).wait_recv()

    def weight_sends(i):
        @pl.loop(1, n_sp)
        def _(off):
            to = lax.rem(sp + off, n_sp)
            lanes = pl.ds(pl.multiple_of(lax.rem(to, n) * cols, cols), cols)
            copy(wloc.at[i, :, lanes], wbuf.at[i, sp, dp], w_s.at[i], w_r.at[i], at_sp(to)).start()

    def weight_wait(sem, i):
        part = wbuf.at[i, pl.ds(0, n_sp - 1), 0]
        pltpu.make_async_copy(part, part, sem.at[i]).wait()

    def weight_relay(i):
        weight_wait(w_r, i)
        part = wbuf.at[i, :, dp]
        for k in range(1, n_dp):
            start(copy(part, part, x_s.at[i, k], x_r.at[i, dp], {"sp": sp, "dp": lax.rem(dp + k, n_dp)}))

    def columns_t(i):
        for k in range(1, n_dp):
            of = lax.rem(dp + n_dp - k, n_dp)
            part = wbuf.at[i, :, of]
            copy(part, part, x_s.at[i, 0], x_r.at[i, of], partner).wait_recv()
        flat = wbuf[i].astype(jnp.float32).reshape(n_sp * n_dp * depth, cols)
        return jnp.transpose(flat).astype(jnp.bfloat16)

    tok_view = (lambda q: toks.at[q], lambda k: tok_s.at[k], lambda q: tok_r.at[q])

    def gat_view(t):
        lanes = pl.ds(t * pair, pair)
        return (lambda q: gat.at[q, :, lanes], lambda k: g_s.at[t, k], lambda q: g_r.at[t, q])

    weight_sends(1)
    weight_sends(0)
    spread(*tok_view)
    weight_sends(2)
    weight_relay(1)
    weight_relay(0)
    for k in range(1, n_dp):
        span = pl.ds(pl.multiple_of(dp * mrows + core * mhalf, mhalf), mhalf)
        start(copy(mbuf.at[span], mbuf.at[span], m_s.at[k], m_r.at[dp * 2 + core],
                   {"sp": sp, "dp": lax.rem(dp + k, n_dp)}))

    both = jnp.concatenate([columns_t(0), columns_t(1)], axis=0)
    for k in range(chips):
        if k + 1 < chips:
            relay(k + 1, *tok_view)
        arrive(k, *tok_view)
        at = lax.rem(chip + chips - k, chips)
        part = toks[pl.ds(at * 2, 2)].reshape(pair, model)
        result = dot_nt(both, part)
        lanes = pl.ds(pl.multiple_of(at * pair, pair), pair)
        ubuf[:, lanes] = result[:cols].astype(jnp.bfloat16)
        v = result[cols:].astype(jnp.bfloat16).astype(jnp.float32)
        vbuf[:, lanes] = v
        total_v = jnp.sum(v, axis=0, keepdims=True)
        away = v - total_v * (1.0 / cols)
        stats[p, 0:1, lanes] = total_v
        stats[p, 1:2, lanes] = jnp.sum(away * away, axis=0, keepdims=True)

    for k in range(1, n):
        start(copy(stats.at[p], stats.at[p], st_s.at[k], st_r.at[p], at_sp(base + lax.rem(p + k, n))))

    for k in range(1, n_dp):
        of = lax.rem(dp + n_dp - k, n_dp)
        span = pl.ds(pl.multiple_of(of * mrows + core * mhalf, mhalf), mhalf)
        one = copy(mbuf.at[span], mbuf.at[span], m_s.at[n_dp - 1 + k], m_r.at[of * 2 + core], partner)
        one.wait_recv()
        start(one)
    weight_relay(2)
    for k in range(1, n_dp):
        of = lax.rem(dp + n_dp - k, n_dp)
        span = pl.ds(pl.multiple_of(of * mrows + (1 - core) * mhalf, mhalf), mhalf)
        copy(mbuf.at[span], mbuf.at[span], m_s.at[0], m_r.at[of * 2 + 1 - core], partner).wait_recv()

    row = lax.broadcasted_iota(jnp.int32, (pair, pair), 0) // SPAN
    col = lax.broadcasted_iota(jnp.int32, (pair, pair), 1) // SPAN
    for t in range(chips):
        lo, hi = t * pair, (t + 1) * pair
        diag = mbuf[lo:hi, lo:hi].astype(jnp.float32)
        dbuf[t] = jnp.where(col <= row, diag, 0.0).astype(jnp.bfloat16)
    gain_t = jnp.transpose(jnp.broadcast_to(gain[:, own], (cols, cols)))[:, 0:1]
    for k in range(1, n):
        slot = lax.rem(p + n - k, n)
        copy(stats.at[slot], stats.at[slot], st_s.at[0], st_r.at[slot], partner).wait_recv()
    sums = [stats[q, 0:1, :] for q in range(n)]
    mean = functools.reduce(jnp.add, sums) * (1.0 / width)
    square = jnp.zeros_like(mean)
    for q in range(n):
        gap = sums[q] * (1.0 / cols) - mean
        square = square + stats[q, 1:2, :] + cols * (gap * gap)
    scale = lax.rsqrt(square * (1.0 / width) + EPS)
    normed = ((vbuf[...] - mean) * scale * gain_t).astype(jnp.bfloat16)

    bias_row = bias[pl.ds(head, 1), :]
    for t in range(chips):
        lo, hi = t * pair, (t + 1) * pair
        mixed = dot_nt(normed[:, lo:hi], dbuf[t])
        if t:
            mixed = mixed + dot_nt(normed[:, :lo], mbuf[lo:hi, :lo])
        mixed = (mixed + bias_row[:, lo:hi]).astype(jnp.bfloat16).astype(jnp.float32)
        gat[p, :, lo:hi] = (ubuf[:, lo:hi].astype(jnp.float32) * mixed).astype(jnp.bfloat16)
        spread(*gat_view(t))

    wo_t = columns_t(2)
    for t in range(chips):
        for k in range(1, chips):
            relay(k, *gat_view(t))
        for k in range(chips):
            arrive(k, *gat_view(t))
        right = gat[:, :, t * pair:(t + 1) * pair].reshape(width, pair)
        result = jnp.dot(wo_t, right, preferred_element_type=jnp.float32)
        turned = jnp.transpose(result).astype(jnp.bfloat16)
        osend[2 * t:2 * t + 2] = turned.reshape(2, rows, cols)
        for q in (2 * t, 2 * t + 1):
            @pl.when(p != q)
            def _():
                copy(osend.at[q], out.at[:, own], o_s.at[q], o_r.at[p], at_sp(base + q)).start()

            @pl.when(p == q)
            def _():
                out[:, own] = osend[q]

    for k in range(1, n):
        slot = lax.rem(p + n - k, n)
        there = out.at[:, pl.ds(pl.multiple_of(slot * cols, cols), cols)]
        copy(osend.at[0], there, o_s.at[0], o_r.at[slot], partner).wait_recv()
    for k in range(1, n):
        q = lax.rem(p + k, n)
        copy(osend.at[q], out.at[:, own], o_s.at[q], o_r.at[p], at_sp(base + q)).wait_send()
    for one in sent:
        one.wait_send()
    for i in range(3):
        weight_wait(w_s, i)


def body(n_sp, n_dp, tokens, proj_gate, proj_value, norm_gain, mix_weight, mix_bias, proj_out):
    rows, model = tokens.shape[1:]
    width = norm_gain.shape[0]
    block = mix_weight.shape[2]
    n = block // rows
    cols = width // n
    depth = proj_gate.shape[0]
    chips = n // 2
    hbm = pl.BlockSpec(memory_space=pltpu.HBM)
    dma = pltpu.SemaphoreType.DMA
    result = pl.pallas_call(
        functools.partial(kernel, n_sp, n_dp),
        out_shape=jax.ShapeDtypeStruct((rows, model), jnp.bfloat16),
        in_specs=[hbm] * 7,
        out_specs=pl.BlockSpec(memory_space=pltpu.VMEM),
        scratch_shapes=[
            pltpu.VMEM((n, rows, model), jnp.bfloat16),
            pltpu.VMEM((3, depth, width), jnp.bfloat16),
            pltpu.VMEM((3, n_sp, n_dp, depth, cols), jnp.bfloat16),
            pltpu.VMEM((block, block), jnp.bfloat16),
            pltpu.VMEM((chips, 2 * rows, 2 * rows), jnp.bfloat16),
            pltpu.VMEM((1, width), jnp.float32),
            pltpu.VMEM(mix_bias.shape, jnp.float32),
            pltpu.VMEM((n, 2, block), jnp.float32),
            pltpu.VMEM((n, cols, block), jnp.bfloat16),
            pltpu.VMEM((cols, block), jnp.bfloat16),
            pltpu.VMEM((cols, block), jnp.float32),
            pltpu.VMEM((n, rows, cols), jnp.bfloat16),
            dma((10,)), dma((n,)), dma((n,)), dma((3,)), dma((3,)),
            dma((3, n_dp)), dma((3, n_dp)), dma((2 * n_dp,)), dma((2 * n_dp,)),
            dma((n,)), dma((n,)), dma((chips, n)), dma((chips, n)), dma((n,)), dma((n,)),
        ],
        compiler_params=pltpu.CompilerParams(
            collective_id=0, has_side_effects=True, vmem_limit_bytes=60 * 1024 * 1024),
    )(tokens.reshape(rows, model), proj_gate, proj_value, norm_gain.reshape(1, width),
      mix_weight, mix_bias, proj_out)
    return result.reshape(1, rows, model)


def solution(mesh):
    return jax.shard_map(
        functools.partial(body, mesh.shape["sp"], mesh.shape["dp"]),
        mesh=mesh,
        in_specs=(
            P("dp", "sp", None),
            P(("sp", "dp"), None),
            P(("sp", "dp"), None),
            P(),
            P(None, "dp", None),
            P(),
            P(("sp", "dp"), None),
        ),
        out_specs=P("dp", "sp", None),
        check_vma=False,
    )
```

```python
import functools

import jax
import jax.numpy as jnp
from jax import lax
from jax.experimental import pallas as pl
from jax.experimental.pallas import tpu as pltpu
from jax.sharding import PartitionSpec as P

HEAD_DIM = 256
SPAN = 64
EPS = 1e-05
NT = (((1,), (1,)), ((), ()))


def dot_nt(left, right):
    return lax.dot_general(left, right, NT, preferred_element_type=jnp.float32)


def kernel(n_sp, n_dp, tok, wg, wv, gain_in, mix, bias_in, wo, out,
           toks, wloc, wbuf, mbuf, dbuf, gain, bias, stats, gat, ubuf, vbuf, osend,
           l_s, tok_s, tok_r, w_s, w_r, x_s, x_r, m_s, m_r, st_s, st_r, g_s, g_r, o_s, o_r):
    rows, model = tok.shape
    width = gain.shape[1]
    block = mix.shape[2]
    n = block // rows
    chips = n // 2
    cols = width // n
    depth = wg.shape[0]
    mrows = mix.shape[1]
    mhalf = mrows // 2
    pair = 2 * rows
    sp, dp = lax.axis_index("sp"), lax.axis_index("dp")
    p = lax.rem(sp, n)
    base = sp - p
    chip, core = lax.div(p, 2), lax.rem(p, 2)
    partner = {"sp": base + chip * 2 + 1 - core, "dp": dp}
    head = lax.div(p * cols, HEAD_DIM)
    own = pl.ds(pl.multiple_of(p * cols, cols), cols)
    mine = pl.ds(pl.multiple_of(dp * mrows, mrows), mrows)

    def copy(src, dst, ssem, rsem, device):
        return pltpu.make_async_remote_copy(
            src_ref=src, dst_ref=dst, send_sem=ssem, recv_sem=rsem,
            device_id=device, device_id_type=pl.DeviceIdType.MESH)

    def at_sp(index):
        return {"sp": index, "dp": dp}

    loads = [(wg, wloc.at[0]), (wv, wloc.at[1]), (wo, wloc.at[2]), (tok, toks.at[p]),
             (gain_in, gain), (bias_in, bias), (mix.at[head], mbuf.at[mine])]
    loads += [(w.at[:, own], wbuf.at[i, sp, dp]) for i, w in enumerate((wg, wv, wo))]
    loads = [pltpu.make_async_copy(src, dst, l_s.at[i]) for i, (src, dst) in enumerate(loads)]
    for one in loads:
        one.start()

    barrier = pltpu.get_barrier_semaphore()

    @pl.loop(1, n_sp)
    def _(off):
        pl.semaphore_signal(barrier, inc=1, device_id=at_sp(lax.rem(sp + off, n_sp)),
                            device_id_type=pl.DeviceIdType.MESH)

    for k in range(1, n_dp):
        pl.semaphore_signal(barrier, inc=1, device_id={"sp": sp, "dp": lax.rem(dp + k, n_dp)},
                            device_id_type=pl.DeviceIdType.MESH)
    pl.semaphore_wait(barrier, n_sp + n_dp - 2)
    for one in loads:
        one.wait()
    sent = []

    def start(one):
        one.start()
        sent.append(one)

    def slot_of(k, side):
        return lax.rem(chip + chips - k, chips) * 2 + side

    def spread(view, ssem, rsem):
        for k in range(1, chips):
            peer = base + lax.rem(chip + k, chips) * 2 + core
            start(copy(view(p), view(p), ssem(k), rsem(p), at_sp(peer)))
        start(copy(view(p), view(p), ssem(0), rsem(p), partner))

    def relay(k, view, ssem, rsem):
        slot = slot_of(k, core)
        one = copy(view(slot), view(slot), ssem(chips - 1 + k), rsem(slot), partner)
        one.wait_recv()
        start(one)

    def arrive(k, view, ssem, rsem):
        slot = slot_of(k, 1 - core)
        copy(view(slot), view(slot), ssem(0), rsem(slot), partner).wait_recv()

    def weight_sends(i):
        @pl.loop(1, n_sp)
        def _(off):
            to = lax.rem(sp + off, n_sp)
            lanes = pl.ds(pl.multiple_of(lax.rem(to, n) * cols, cols), cols)
            copy(wloc.at[i, :, lanes], wbuf.at[i, sp, dp], w_s.at[i], w_r.at[i], at_sp(to)).start()

    def weight_wait(sem, i):
        part = wbuf.at[i, pl.ds(0, n_sp - 1), 0]
        pltpu.make_async_copy(part, part, sem.at[i]).wait()

    def weight_relay(i):
        weight_wait(w_r, i)
        part = wbuf.at[i, :, dp]
        for k in range(1, n_dp):
            start(copy(part, part, x_s.at[i, k], x_r.at[i, dp], {"sp": sp, "dp": lax.rem(dp + k, n_dp)}))

    def columns_t(i):
        for k in range(1, n_dp):
            of = lax.rem(dp + n_dp - k, n_dp)
            part = wbuf.at[i, :, of]
            copy(part, part, x_s.at[i, 0], x_r.at[i, of], partner).wait_recv()
        flat = wbuf[i].astype(jnp.float32).reshape(n_sp * n_dp * depth, cols)
        return jnp.transpose(flat).astype(jnp.bfloat16)

    tok_view = (lambda q: toks.at[q], lambda k: tok_s.at[k], lambda q: tok_r.at[q])

    def gat_view(t):
        lanes = pl.ds(t * pair, pair)
        return (lambda q: gat.at[q, :, lanes], lambda k: g_s.at[t, k], lambda q: g_r.at[t, q])

    quarter = mhalf // 2

    def mix_span(of, side, piece):
        return pl.ds(pl.multiple_of(of * mrows + side * mhalf + piece * quarter, quarter), quarter)

    def mix_send(piece):
        span = mix_span(dp, core, piece)
        for k in range(1, n_dp):
            start(copy(mbuf.at[span], mbuf.at[span], m_s.at[piece, k], m_r.at[piece, dp * 2 + core],
                       {"sp": sp, "dp": lax.rem(dp + k, n_dp)}))

    def mix_relay(piece):
        for k in range(1, n_dp):
            of = lax.rem(dp + n_dp - k, n_dp)
            span = mix_span(of, core, piece)
            one = copy(mbuf.at[span], mbuf.at[span], m_s.at[piece, n_dp - 1 + k],
                       m_r.at[piece, of * 2 + core], partner)
            one.wait_recv()
            start(one)

    def mix_arrive(piece):
        for k in range(1, n_dp):
            of = lax.rem(dp + n_dp - k, n_dp)
            span = mix_span(of, 1 - core, piece)
            copy(mbuf.at[span], mbuf.at[span], m_s.at[piece, 0],
                 m_r.at[piece, of * 2 + 1 - core], partner).wait_recv()

    mix_send(0)
    weight_sends(1)
    weight_sends(0)
    spread(*tok_view)
    weight_relay(1)
    weight_relay(0)
    mix_send(1)

    both = jnp.concatenate([columns_t(0), columns_t(1)], axis=0)
    for k in range(chips):
        if k + 1 < chips:
            relay(k + 1, *tok_view)
        arrive(k, *tok_view)
        at = lax.rem(chip + chips - k, chips)
        part = toks[pl.ds(at * 2, 2)].reshape(pair, model)
        result = dot_nt(both, part)
        lanes = pl.ds(pl.multiple_of(at * pair, pair), pair)
        ubuf[:, lanes] = result[:cols].astype(jnp.bfloat16)
        v = result[cols:].astype(jnp.bfloat16).astype(jnp.float32)
        vbuf[:, lanes] = v
        total_v = jnp.sum(v, axis=0, keepdims=True)
        away = v - total_v * (1.0 / cols)
        stats[p, 0:1, lanes] = total_v
        stats[p, 1:2, lanes] = jnp.sum(away * away, axis=0, keepdims=True)

    for k in range(1, n):
        start(copy(stats.at[p], stats.at[p], st_s.at[k], st_r.at[p], at_sp(base + lax.rem(p + k, n))))

    weight_sends(2)
    for piece in range(2):
        mix_relay(piece)
    for piece in range(2):
        mix_arrive(piece)

    row = lax.broadcasted_iota(jnp.int32, (pair, pair), 0) // SPAN
    col = lax.broadcasted_iota(jnp.int32, (pair, pair), 1) // SPAN
    for t in range(chips):
        lo, hi = t * pair, (t + 1) * pair
        diag = mbuf[lo:hi, lo:hi].astype(jnp.float32)
        dbuf[t] = jnp.where(col <= row, diag, 0.0).astype(jnp.bfloat16)
    gain_t = jnp.transpose(jnp.broadcast_to(gain[:, own], (cols, cols)))[:, 0:1]
    for k in range(1, n):
        slot = lax.rem(p + n - k, n)
        copy(stats.at[slot], stats.at[slot], st_s.at[0], st_r.at[slot], partner).wait_recv()
    sums = [stats[q, 0:1, :] for q in range(n)]
    mean = functools.reduce(jnp.add, sums) * (1.0 / width)
    square = jnp.zeros_like(mean)
    for q in range(n):
        gap = sums[q] * (1.0 / cols) - mean
        square = square + stats[q, 1:2, :] + cols * (gap * gap)
    scale = lax.rsqrt(square * (1.0 / width) + EPS)
    normed = ((vbuf[...] - mean) * scale * gain_t).astype(jnp.bfloat16)

    bias_row = bias[pl.ds(head, 1), :]
    for t in range(chips):
        lo, hi = t * pair, (t + 1) * pair
        mixed = dot_nt(normed[:, lo:hi], dbuf[t])
        if t:
            mixed = mixed + dot_nt(normed[:, :lo], mbuf[lo:hi, :lo])
        mixed = (mixed + bias_row[:, lo:hi]).astype(jnp.bfloat16).astype(jnp.float32)
        gat[p, :, lo:hi] = (ubuf[:, lo:hi].astype(jnp.float32) * mixed).astype(jnp.bfloat16)
        spread(*gat_view(t))
        if t == 1:
            weight_relay(2)

    wo_t = columns_t(2)
    for t in range(chips):
        for k in range(1, chips):
            relay(k, *gat_view(t))
        for k in range(chips):
            arrive(k, *gat_view(t))
        right = gat[:, :, t * pair:(t + 1) * pair].reshape(width, pair)
        result = jnp.dot(wo_t, right, preferred_element_type=jnp.float32)
        turned = jnp.transpose(result).astype(jnp.bfloat16)
        osend[2 * t:2 * t + 2] = turned.reshape(2, rows, cols)
        for q in (2 * t, 2 * t + 1):
            @pl.when(p != q)
            def _():
                copy(osend.at[q], out.at[:, own], o_s.at[q], o_r.at[p], at_sp(base + q)).start()

            @pl.when(p == q)
            def _():
                out[:, own] = osend[q]

    for k in range(1, n):
        slot = lax.rem(p + n - k, n)
        there = out.at[:, pl.ds(pl.multiple_of(slot * cols, cols), cols)]
        copy(osend.at[0], there, o_s.at[0], o_r.at[slot], partner).wait_recv()
    for k in range(1, n):
        q = lax.rem(p + k, n)
        copy(osend.at[q], out.at[:, own], o_s.at[q], o_r.at[p], at_sp(base + q)).wait_send()
    for one in sent:
        one.wait_send()
    for i in range(3):
        weight_wait(w_s, i)


def body(n_sp, n_dp, tokens, proj_gate, proj_value, norm_gain, mix_weight, mix_bias, proj_out):
    rows, model = tokens.shape[1:]
    width = norm_gain.shape[0]
    block = mix_weight.shape[2]
    n = block // rows
    cols = width // n
    depth = proj_gate.shape[0]
    chips = n // 2
    hbm = pl.BlockSpec(memory_space=pltpu.HBM)
    dma = pltpu.SemaphoreType.DMA
    result = pl.pallas_call(
        functools.partial(kernel, n_sp, n_dp),
        out_shape=jax.ShapeDtypeStruct((rows, model), jnp.bfloat16),
        in_specs=[hbm] * 7,
        out_specs=pl.BlockSpec(memory_space=pltpu.VMEM),
        scratch_shapes=[
            pltpu.VMEM((n, rows, model), jnp.bfloat16),
            pltpu.VMEM((3, depth, width), jnp.bfloat16),
            pltpu.VMEM((3, n_sp, n_dp, depth, cols), jnp.bfloat16),
            pltpu.VMEM((block, block), jnp.bfloat16),
            pltpu.VMEM((chips, 2 * rows, 2 * rows), jnp.bfloat16),
            pltpu.VMEM((1, width), jnp.float32),
            pltpu.VMEM(mix_bias.shape, jnp.float32),
            pltpu.VMEM((n, 2, block), jnp.float32),
            pltpu.VMEM((n, cols, block), jnp.bfloat16),
            pltpu.VMEM((cols, block), jnp.bfloat16),
            pltpu.VMEM((cols, block), jnp.float32),
            pltpu.VMEM((n, rows, cols), jnp.bfloat16),
            dma((10,)), dma((n,)), dma((n,)), dma((3,)), dma((3,)),
            dma((3, n_dp)), dma((3, n_dp)), dma((2, 2 * n_dp)), dma((2, 2 * n_dp)),
            dma((n,)), dma((n,)), dma((chips, n)), dma((chips, n)), dma((n,)), dma((n,)),
        ],
        compiler_params=pltpu.CompilerParams(
            collective_id=0, has_side_effects=True, vmem_limit_bytes=60 * 1024 * 1024),
    )(tokens.reshape(rows, model), proj_gate, proj_value, norm_gain.reshape(1, width),
      mix_weight, mix_bias, proj_out)
    return result.reshape(1, rows, model)


def solution(mesh):
    return jax.shard_map(
        functools.partial(body, mesh.shape["sp"], mesh.shape["dp"]),
        mesh=mesh,
        in_specs=(
            P("dp", "sp", None),
            P(("sp", "dp"), None),
            P(("sp", "dp"), None),
            P(),
            P(None, "dp", None),
            P(),
            P(("sp", "dp"), None),
        ),
        out_specs=P("dp", "sp", None),
        check_vma=False,
    )
```
